32 devices in a mesh: sp: 8 (over z, x), tp: 4 (over y, core).
Axes of the slice: x: 2, y: 2, z: 4, core: 2. Of those that a mesh axis runs over, the one named last changes fastest.
Arguments:
- tokens: bfloat16 [2048, 2048], P('sp'), may hold values from -6 to 6
- documents: int32 [2048], P('sp'), may hold values from 0 to 3, never falling along the last dimension, each value on 1 to 1024 neighbouring positions
- norm_gain: float32 [1, 2048], replicated, may hold values from 0.1 to 1.9
- w_query: bfloat16 [1, 2048, 2048], P(None, 'sp', 'tp'), may hold values from -0.125 to 0.125
- w_key: bfloat16 [1, 2048, 2048], P(None, 'sp', 'tp'), may hold values from -0.125 to 0.125
- w_value: bfloat16 [1, 2048, 2048], P(None, 'sp', 'tp'), may hold values from -0.125 to 0.125
- w_out: bfloat16 [1, 2048, 2048], P(None, None, 'sp'), may hold values from -0.59765625 to 0.59765625
- rel_bias: float32 [1, 32, 257], P(None, 'tp'), may hold values from -8 to 240
Outputs:
- mixed: bfloat16 [2048, 2048], P('sp')
The draws below stay inside these ranges and needn't reach their ends.
Inputs may be any that keep to these rules, and one draw needn't show every extreme that they name: `documents`: document numbers never fall along the sequence; a document has 1 to 1024 positions.
All inputs are finite; a program needn't handle non-finite values.
Results may differ from the reference program's by a relative error of at most 0.007.
Values may be sent and summed in bfloat16 or wider, within the bound.
A program may use at most 128 MiB of HBM per device.

```python
import math
import jax
import jax.numpy as jnp
import numpy as np
from jax import lax

D = 2048
HEADS = 32
HEAD_DIM = 64
SEG = 64
LEFT = 4
REL_CLIP = 128
LAYERS = 1
TOK_DEV = 256
TOKENS = 2048
DOC_SPAN = 1024
N_SP = 8


def draw_rel_bias(key, part):
    bias_shape = (LAYERS, HEADS, 2 * REL_CLIP + 1)
    base_draw = jnp.clip(jax.random.normal(key, bias_shape, jnp.float32) * 1.5, -8.0, 8.0)
    return base_draw


def block_scale(key, dims, split, low, high):
    def one(dim, blocks):
        heights = jax.random.uniform(jax.random.fold_in(jax.random.fold_in(key, 6), dim), (blocks,), jnp.float32, low / len(split), high / len(split))
        return jnp.repeat(jnp.exp(heights), dims[dim] // blocks).reshape((-1,) + (1,) * (len(dims) - dim - 1))

    gain = one(*split[0])
    for cut in split[1:]:
        gain = gain * one(*cut)
    return gain


def profile(amount, total, bound, slope):
    portions = [(1 << 20) // math.isqrt(standing ** slope) + 1 for standing in range(2, amount + 1)]
    spare, holding = total - bound - (amount - 1), [1] * (amount - 1)
    while spare > 0:
        candidates = [i for i in range(amount - 1) if holding[i] < bound]
        mass, left = sum([portions[i] for i in candidates]), spare
        for i in candidates:
            addition = min(bound - holding[i], max(1, left * portions[i] // mass), spare)
            holding[i] = holding[i] + addition
            spare = spare - addition
    return np.array([bound] + holding)


def ragged_sizes(rng, number_of, total, limit, lean):
    if number_of == 2:
        one = jax.random.randint(rng, (), max(1, total - limit), min(limit, total - 1) + 1)
        return jnp.stack([one, total - one])
    lengths = jnp.asarray(profile(number_of, total, limit, lean), jnp.int32)
    pairs = (number_of - 1) // 2
    source_of, receiver = lengths[1:1 + 2 * pairs:2], lengths[2:2 + 2 * pairs:2]
    slack = jnp.minimum(source_of - 1, limit - receiver)
    passed = jax.random.randint(jax.random.fold_in(rng, 1), (pairs,), 0, 1 << 20) % (slack + 1)
    lengths = lengths.at[1:1 + 2 * pairs:2].set(source_of - passed).at[2:2 + 2 * pairs:2].set(receiver + passed)
    return lengths[jax.random.permutation(jax.random.fold_in(rng, 2), number_of)]


def normal_values(stream_key, extent, width, limit, shards=(), held_as=jnp.bfloat16):
    drawn = width * jax.random.normal(stream_key, extent, jnp.float32)
    if shards:
        drawn = drawn * block_scale(stream_key, extent, shards, -0.22, 0.18)
    return jnp.clip(drawn, -limit, limit).astype(held_as)


def setup_inputs(seed: int = 0) -> dict:
    keys = jax.random.split(jax.random.key(seed), 9)
    tokens = normal_values(keys[0], (TOKENS, D), 1.0, 6.0, ((0, 8),))
    documents = jnp.searchsorted(jnp.cumsum(ragged_sizes(keys[1], N_SP // 2, TOKENS, DOC_SPAN, 0)), jnp.arange(TOKENS), side="right").astype(jnp.int32)
    norm_gain = jnp.clip(1.0 + 0.18 * jax.random.normal(keys[2], (LAYERS, D), jnp.float32), 0.1, 1.9)
    w_query = normal_values(keys[3], (LAYERS, D, HEADS * HEAD_DIM), D ** -0.5, 0.125, ((1, 8), (2, 4)))
    w_key = normal_values(keys[4], (LAYERS, D, HEADS * HEAD_DIM), D ** -0.5, 0.125, ((1, 8), (2, 4)))
    w_value = normal_values(keys[5], (LAYERS, D, HEADS * HEAD_DIM), D ** -0.5, 0.125, ((1, 8), (2, 4)))
    w_out = normal_values(keys[6], (LAYERS, HEADS * HEAD_DIM, D), 0.1, 0.59765625, ((2, 8),))
    rel_bias = draw_rel_bias(jax.random.fold_in(keys[8], 71), 0)
    return dict(tokens=tokens, documents=documents, norm_gain=norm_gain, w_query=w_query, w_key=w_key, w_value=w_value, w_out=w_out, rel_bias=rel_bias)


EPS = 1e-06

def attend(queries, keys_all, values_all, query_pos, key_pos, query_doc, key_doc, bias_table):
    scores = jnp.einsum('qhe,khe->hqk', queries.astype(jnp.float32), keys_all.astype(jnp.float32)) * HEAD_DIM ** (-0.5)
    distance = jnp.clip(query_pos[:, None] - key_pos[None, :], -REL_CLIP, REL_CLIP) + REL_CLIP
    scores = scores + jnp.take(bias_table, distance, axis=1)
    query_seg = query_pos // SEG
    key_seg = key_pos // SEG
    allowed = (key_pos[None, :] >= 0) & (key_seg[None, :] <= query_seg[:, None]) & (key_seg[None, :] >= query_seg[:, None] - LEFT) & (key_doc[None, :] == query_doc[:, None])
    scores = jnp.where(allowed[None], scores, -1e+30)
    peak = lax.optimization_barrier(jnp.max(scores, axis=-1, keepdims=True))
    raised = jnp.exp(scores - peak)
    weights_bf = (raised / lax.optimization_barrier(jnp.sum(raised, axis=-1, keepdims=True))).astype(jnp.bfloat16)
    return jnp.einsum('hqk,khe->qhe', weights_bf.astype(jnp.float32), values_all.astype(jnp.float32)).astype(jnp.bfloat16)

def reference(tokens, documents, norm_gain, w_query, w_key, w_value, w_out, rel_bias):
    reach_rows = LEFT * SEG
    block_count = TOKENS // TOK_DEV
    current = tokens
    doc_pad = jnp.concatenate([jnp.zeros((reach_rows,), jnp.int32), documents.astype(jnp.int32)])
    for depth_index in range(LAYERS):
        widened = current.astype(jnp.float32)
        normed = (widened * lax.rsqrt(lax.optimization_barrier(jnp.mean(widened * widened, axis=-1, keepdims=True)) + EPS) * norm_gain[depth_index]).astype(jnp.bfloat16)
        queries = jnp.dot(normed, w_query[depth_index], preferred_element_type=jnp.float32).astype(jnp.bfloat16).reshape(TOKENS, HEADS, HEAD_DIM)
        keys_all = jnp.dot(normed, w_key[depth_index], preferred_element_type=jnp.float32).astype(jnp.bfloat16).reshape(TOKENS, HEADS, HEAD_DIM)
        values_all = jnp.dot(normed, w_value[depth_index], preferred_element_type=jnp.float32).astype(jnp.bfloat16).reshape(TOKENS, HEADS, HEAD_DIM)
        zero_rows = jnp.zeros((reach_rows, HEADS, HEAD_DIM), jnp.bfloat16)
        key_pad = jnp.concatenate([zero_rows, keys_all], axis=0)
        value_pad = jnp.concatenate([zero_rows, values_all], axis=0)
        bias_table = rel_bias[depth_index]

        def one_block(block_index):
            first_row = (block_index * TOK_DEV).astype(jnp.int32)
            query_block = lax.dynamic_slice_in_dim(queries, first_row, TOK_DEV, 0)
            key_block = lax.dynamic_slice_in_dim(key_pad, first_row, reach_rows + TOK_DEV, 0)
            value_block = lax.dynamic_slice_in_dim(value_pad, first_row, reach_rows + TOK_DEV, 0)
            query_doc = lax.dynamic_slice_in_dim(documents, first_row, TOK_DEV, 0)
            key_doc = lax.dynamic_slice_in_dim(doc_pad, first_row, reach_rows + TOK_DEV, 0)
            query_pos = first_row + jnp.arange(TOK_DEV, dtype=jnp.int32)
            key_pos = first_row - reach_rows + jnp.arange(reach_rows + TOK_DEV, dtype=jnp.int32)
            return attend(query_block, key_block, value_block, query_pos, key_pos, query_doc, key_doc, bias_table)
        attended = lax.map(one_block, jnp.arange(block_count, dtype=jnp.int32)).reshape(TOKENS, HEADS * HEAD_DIM)
        product = jnp.dot(attended, w_out[depth_index], preferred_element_type=jnp.float32)
        current = (widened + product).astype(jnp.bfloat16)
    return current
```

```python
import functools

import jax
import jax.numpy as jnp
from jax import lax
from jax.experimental import pallas as pl
from jax.experimental.pallas import tpu as pltpu
from jax.sharding import PartitionSpec as P

HEAD_DIM = 64
SEG = 64
LEFT = 4
REL_CLIP = 128


EPS = 1e-06


def passed_along(x, axis, by):
    length = lax.axis_size(axis)
    pairs = [(i, i + by) for i in range(length) if 0 <= i + by < length]
    return lax.ppermute(x, axis, pairs)


def banded_bias(bias_table, query_rows, key_rows, reach_rows):
    span_len = query_rows + key_rows - 1
    steps_back = jnp.arange(span_len, dtype=jnp.int32) - (key_rows - 1) + reach_rows
    lookup = jnp.clip(steps_back, -REL_CLIP, REL_CLIP) + REL_CLIP
    bias_line = jnp.take(bias_table, lookup, axis=1)
    reversed_line = bias_line[:, ::-1]
    repeated = jnp.tile(reversed_line, (1, query_rows))
    skewed = repeated[:, query_rows - 1 : query_rows - 1 + query_rows * (span_len - 1)]
    skewed = skewed.reshape(bias_table.shape[0], query_rows, span_len - 1)
    return skewed[:, :, :key_rows]


def attend(queries, keys_all, values_all, query_pos, key_pos, query_doc, key_doc, bias_table):
    query_rows = queries.shape[0]
    key_rows = keys_all.shape[0]
    reach_rows = key_rows - query_rows
    scores = jnp.einsum(
        "qhe,khe->hqk", queries, keys_all, preferred_element_type=jnp.float32
    ) * HEAD_DIM ** (-0.5)
    scores = scores + banded_bias(bias_table, query_rows, key_rows, reach_rows)
    query_seg = query_pos // SEG
    key_seg = key_pos // SEG
    allowed = (
        (key_pos[None, :] >= 0)
        & (key_seg[None, :] <= query_seg[:, None])
        & (key_seg[None, :] >= query_seg[:, None] - LEFT)
        & (key_doc[None, :] == query_doc[:, None])
    )
    scores = jnp.where(allowed[None], scores, -1e30)
    peak = jnp.max(scores, axis=-1, keepdims=True)
    raised = jnp.exp(scores - peak)
    weights_bf = (raised / jnp.sum(raised, axis=-1, keepdims=True)).astype(jnp.bfloat16)
    return jnp.einsum(
        "hqk,khe->qhe", weights_bf, values_all, preferred_element_type=jnp.float32
    ).astype(jnp.bfloat16)


def body(tokens, documents, norm_gain, w_query, w_key, w_value, w_out, rel_bias):
    local_rows = tokens.shape[0]
    reach_rows = LEFT * SEG
    width_local = w_query.shape[2]
    heads_local = width_local // HEAD_DIM
    offset = lax.axis_index("sp") * local_rows
    query_pos = offset + jnp.arange(local_rows, dtype=jnp.int32)
    key_pos = offset - reach_rows + jnp.arange(reach_rows + local_rows, dtype=jnp.int32)
    widened = tokens.astype(jnp.float32)
    normed = (
        widened
        * lax.rsqrt(jnp.mean(widened * widened, axis=-1, keepdims=True) + EPS)
        * norm_gain[0]
    ).astype(jnp.bfloat16)
    query_sum = jnp.dot(
        normed,
        lax.all_gather(w_query[0], "sp", axis=0, tiled=True),
        preferred_element_type=jnp.float32,
    )
    key_sum = jnp.dot(
        normed,
        lax.all_gather(w_key[0], "sp", axis=0, tiled=True),
        preferred_element_type=jnp.float32,
    )
    value_sum = jnp.dot(
        normed,
        lax.all_gather(w_value[0], "sp", axis=0, tiled=True),
        preferred_element_type=jnp.float32,
    )
    queries = query_sum.astype(jnp.bfloat16)
    keys_own = key_sum.astype(jnp.bfloat16)
    values_own = value_sum.astype(jnp.bfloat16)
    prior_keys, prior_values, prior_docs = passed_along((keys_own, values_own, documents), "sp", 1)
    keys_all = jnp.concatenate([prior_keys, keys_own], axis=0)
    values_all = jnp.concatenate([prior_values, values_own], axis=0)
    key_doc = jnp.concatenate([prior_docs, documents], axis=0)
    attended = attend(
        queries.reshape(local_rows, heads_local, HEAD_DIM),
        keys_all.reshape(reach_rows + local_rows, heads_local, HEAD_DIM),
        values_all.reshape(reach_rows + local_rows, heads_local, HEAD_DIM),
        query_pos,
        key_pos,
        documents,
        key_doc,
        rel_bias[0],
    ).reshape(local_rows, width_local)
    all_heads = lax.all_gather(attended, "tp", axis=1, tiled=True)
    return (
        widened
        + jnp.dot(
            all_heads,
            lax.all_gather(w_out[0], "sp", axis=1, tiled=True),
            preferred_element_type=jnp.float32,
        )
    ).astype(jnp.bfloat16)


MESH = pl.DeviceIdType.MESH
KEY, VALUE, QUERY, OUT = range(4)
UP, DOWN, ACROSS = range(3)
NEG = -1e30


def layer_kernel(
    n_sp, n_tp, x_ref, doc_col, doc_row, gain_ref, line_ref, wk_in, wv_in, wq_in, wo_in, out_ref,
    w_all, wo_all, normed, bias, q_buf, k_all, v_all, docs_all, att, part_out, part_in, hop_out, hop_in, done,
    own_sem, send_sem, recv_sem, halo_send, halo_recv, tp_send, tp_recv, store_sem,
):
    rows, width = x_ref.shape
    depth, cols = wk_in.shape
    chunk = width // n_tp
    lanes = 2 * HEAD_DIM
    nz = n_sp // 2
    s = lax.axis_index("sp")
    t = lax.axis_index("tp")
    z, x = s // 2, s % 2
    mate = s + 1 - 2 * x
    ty, tc = t // 2, t % 2
    t_core = t + 1 - 2 * tc
    t_y = (1 - ty) * 2 + tc
    own_in = (wk_in, wv_in, wq_in)

    def slot(kind, block):
        if kind == OUT:
            return wo_all.at[block]
        return w_all.at[kind, pl.ds(pl.multiple_of(block * depth, depth), depth), :]

    def own_copy(kind):
        if kind == OUT:
            src = wo_in.at[pl.ds(pl.multiple_of(t * cols, cols), cols), :]
        else:
            src = own_in[kind]
        return pltpu.make_async_copy(src, slot(kind, s), own_sem.at[kind])

    for kind in range(4):
        own_copy(kind).start()

    def move(way, kind, block):
        target = (s + 2, s - 2, mate)[way]
        return pltpu.make_async_remote_copy(
            src_ref=slot(kind, block), dst_ref=slot(kind, block),
            send_sem=send_sem.at[way, kind, block], recv_sem=recv_sem.at[kind, block],
            device_id={"sp": target}, device_id_type=MESH,
        )

    def halo(i):
        buf = (k_all, v_all, docs_all)[i]
        if i == 2:
            src, dst = buf.at[:, pl.ds(rows, rows)], buf.at[:, pl.ds(0, rows)]
        else:
            src, dst = buf.at[pl.ds(rows, rows), :], buf.at[pl.ds(0, rows), :]
        return pltpu.make_async_remote_copy(
            src_ref=src, dst_ref=dst, send_sem=halo_send.at[i], recv_sem=halo_recv.at[i],
            device_id={"sp": s + 1}, device_id_type=MESH,
        )

    has_up, has_down = z < nz - 1, z > 0
    has_next, has_prior = s < n_sp - 1, s > 0

    barrier = pltpu.get_barrier_semaphore()
    for by in (1, 2, n_sp - 2, n_sp - 1):
        pl.semaphore_signal(barrier, inc=1, device_id={"sp": lax.rem(s + by, n_sp)}, device_id_type=MESH)
    for by in range(1, n_tp):
        pl.semaphore_signal(barrier, inc=1, device_id={"tp": lax.rem(t + by, n_tp)}, device_id_type=MESH)
    pl.semaphore_wait(barrier, 4 + n_tp - 1)

    def send_own(kind):
        own_copy(kind).wait()
        pl.when(has_up)(lambda: move(UP, kind, s).start())
        pl.when(has_down)(lambda: move(DOWN, kind, s).start())
        move(ACROSS, kind, s).start()

    def forward(kind):
        for d in range(1, nz):
            @pl.when(z - d >= 0)
            def _():
                block = s - 2 * d
                move(UP, kind, block).wait_recv()
                pl.when(has_up)(lambda: move(UP, kind, block).start())
                move(ACROSS, kind, block).start()

            @pl.when(z + d < nz)
            def _():
                block = s + 2 * d
                move(DOWN, kind, block).wait_recv()
                pl.when(has_down)(lambda: move(DOWN, kind, block).start())
                move(ACROSS, kind, block).start()

    def arrived_across(kind):
        for d in range(nz):
            move(ACROSS, kind, 2 * d + 1 - x).wait_recv()

    send_own(KEY)
    send_own(VALUE)

    docs_all[:, pl.ds(rows, rows)] = doc_row[...]
    wide = x_ref[...].astype(jnp.float32)
    normed[...] = (
        wide * lax.rsqrt(jnp.mean(wide * wide, axis=-1, keepdims=True) + EPS) * gain_ref[...]
    ).astype(jnp.bfloat16)

    @pl.when(s == 0)
    def _():
        docs_all[:, pl.ds(0, rows)] = jnp.full((8, rows), -1, jnp.int32)
        k_all[pl.ds(0, rows), :] = jnp.zeros((rows, cols), jnp.bfloat16)
        v_all[pl.ds(0, rows), :] = jnp.zeros((rows, cols), jnp.bfloat16)

    q_rows, span = 2 * SEG, (LEFT + 2) * SEG
    q_seg = lax.broadcasted_iota(jnp.int32, (q_rows, span), 0) // SEG
    k_seg = lax.broadcasted_iota(jnp.int32, (q_rows, span), 1) // SEG
    near = (k_seg >= q_seg) & (k_seg <= q_seg + LEFT)
    for h in range(cols // HEAD_DIM):
        line = jnp.broadcast_to(line_ref[pl.ds(h, 1), :], (q_rows, line_ref.shape[1]))
        skew = pltpu.roll(line, 0, 1, stride=1, stride_axis=0)
        bias[h] = jnp.where(near, skew[:, :span], NEG)

    pl.when(has_next)(lambda: halo(2).start())

    def project(kind):
        return jnp.dot(normed[...], w_all[kind], preferred_element_type=jnp.float32)

    forward(KEY)
    send_own(QUERY)
    forward(VALUE)
    arrived_across(KEY)
    k_all[pl.ds(rows, rows), :] = project(KEY).astype(jnp.bfloat16)
    forward(QUERY)
    pl.when(has_next)(lambda: halo(0).start())
    send_own(OUT)
    arrived_across(VALUE)
    v_all[pl.ds(rows, rows), :] = project(VALUE).astype(jnp.bfloat16)
    forward(OUT)
    pl.when(has_next)(lambda: halo(1).start())
    arrived_across(QUERY)
    q_buf[...] = (project(QUERY).astype(jnp.bfloat16).astype(jnp.float32) * HEAD_DIM ** (-0.5)).astype(jnp.bfloat16)

    @pl.when(has_prior)
    def _():
        for i in range(3):
            halo(i).wait_recv()

    low = lax.broadcasted_iota(jnp.int32, (q_rows, lanes), 1) < HEAD_DIM
    for j in range(rows // q_rows):
        same = doc_col[pl.ds(j * q_rows, q_rows), :][:, :1] == docs_all[pl.ds(0, 1), pl.ds(j * q_rows, span)]
        for p in range(cols // lanes):
            q_pair = q_buf[pl.ds(j * q_rows, q_rows), pl.ds(p * lanes, lanes)]
            k_pair = k_all[pl.ds(j * q_rows, span), pl.ds(p * lanes, lanes)]
            v_pair = v_all[pl.ds(j * q_rows, span), pl.ds(p * lanes, lanes)]
            both = []
            for half in range(2):
                mine = low if half == 0 else jnp.logical_not(low)
                q_one = jnp.where(mine, q_pair, jnp.zeros_like(q_pair))
                score = lax.dot_general(
                    q_one, k_pair, (((1,), (1,)), ((), ())), preferred_element_type=jnp.float32
                )
                score = jnp.where(same, score + bias[2 * p + half], NEG)
                raised = jnp.exp(score - jnp.max(score, axis=-1, keepdims=True))
                total = jnp.sum(raised, axis=-1, keepdims=True)
                both.append(
                    jnp.dot(raised.astype(jnp.bfloat16), v_pair, preferred_element_type=jnp.float32) / total
                )
            att[pl.ds(j * q_rows, q_rows), pl.ds(p * lanes, lanes)] = jnp.where(low, both[0], both[1]).astype(jnp.bfloat16)

    arrived_across(OUT)

    def product(block):
        return jnp.dot(att[...], wo_all[block], preferred_element_type=jnp.float32)

    def chunk_product(which):
        each = chunk // wo_in.shape[1]
        return jnp.concatenate([product(which * each + i) for i in range(each)], axis=1)

    def tp_move(i, src, dst, target):
        return pltpu.make_async_remote_copy(
            src_ref=src, dst_ref=dst, send_sem=tp_send.at[i], recv_sem=tp_recv.at[i],
            device_id={"tp": target}, device_id_type=MESH,
        )

    part_moves = [tp_move(i, part_out.at[i], part_in.at[i], t_core) for i in range(2)]
    for i in range(2):
        other = (1 - ty if i == 0 else ty) * 2 + (1 - tc)
        part_out[i] = chunk_product(other).astype(jnp.bfloat16)
        part_moves[i].start()
    far = chunk_product(t_y)
    part_moves[0].wait_recv()
    hop_out[...] = (far + part_in[0].astype(jnp.float32)).astype(jnp.bfloat16)
    hop = tp_move(2, hop_out, hop_in, t_y)
    hop.start()
    near_sum = chunk_product(t)
    part_moves[1].wait_recv()
    near_sum = near_sum + part_in[1].astype(jnp.float32)
    near_sum = near_sum + x_ref[:, pl.ds(pl.multiple_of(t * chunk, chunk), chunk)].astype(jnp.float32)
    hop.wait_recv()
    done[t] = (near_sum + hop_in[...].astype(jnp.float32)).astype(jnp.bfloat16)

    def store(which):
        return pltpu.make_async_copy(
            done.at[which], out_ref.at[:, pl.ds(pl.multiple_of(which * chunk, chunk), chunk)], store_sem.at[which]
        )

    far_core = (1 - ty) * 2 + (1 - tc)
    to_y = tp_move(3, done.at[t], done.at[t], t_y)
    to_core = tp_move(4, done.at[t], done.at[t], t_core)
    pass_on = tp_move(5, done.at[t_y], done.at[t_y], t_core)
    to_y.start()
    to_core.start()
    store(t).start()
    to_y.wait_recv()
    pass_on.start()
    store(t_y).start()
    to_core.wait_recv()
    store(t_core).start()
    pass_on.wait_recv()
    store(far_core).start()
    for which in range(n_tp):
        store(which).wait()

    for kind in range(4):
        for d in range(nz):
            @pl.when(z - d >= 0)
            def _():
                pl.when(has_up)(lambda: move(UP, kind, s - 2 * d).wait_send())
                move(ACROSS, kind, s - 2 * d).wait_send()

            @pl.when(z + d < nz)
            def _():
                pl.when(has_down)(lambda: move(DOWN, kind, s + 2 * d).wait_send())
                if d:
                    move(ACROSS, kind, s + 2 * d).wait_send()
    @pl.when(has_next)
    def _():
        for i in range(3):
            halo(i).wait_send()
    for one in (*part_moves, hop, to_y, to_core, pass_on):
        one.wait_send()


def body_one(n_sp, n_tp, tokens, documents, norm_gain, w_query, w_key, w_value, w_out, rel_bias):
    rows, width = tokens.shape
    depth, cols = w_query.shape[1:]
    heads = cols // HEAD_DIM
    out_cols = w_out.shape[2]
    chunk = width // n_tp
    reach = LEFT * SEG
    table = rel_bias[0]
    furthest = table[:, 2 * REL_CLIP:]
    ahead, behind = reach - REL_CLIP, reach - REL_CLIP - 1
    line = jnp.concatenate(
        [
            jnp.broadcast_to(furthest, (heads, ahead)),
            table[:, ::-1],
            jnp.broadcast_to(furthest, (heads, behind)),
        ],
        axis=1,
    )
    doc_col = jnp.broadcast_to(documents[:, None], (rows, 128))
    doc_row = jnp.broadcast_to(documents[None, :], (8, rows))
    bf, f32 = jnp.bfloat16, jnp.float32
    vmem = pl.BlockSpec(memory_space=pltpu.VMEM)
    hbm = pl.BlockSpec(memory_space=pl.ANY)
    dma = pltpu.SemaphoreType.DMA
    return pl.pallas_call(
        functools.partial(layer_kernel, n_sp, n_tp),
        out_shape=jax.ShapeDtypeStruct((rows, width), bf),
        in_specs=[vmem] * 5 + [hbm] * 4,
        out_specs=hbm,
        scratch_shapes=[
            pltpu.VMEM((3, n_sp * depth, cols), bf),
            pltpu.VMEM((n_sp, cols, out_cols), bf),
            pltpu.VMEM((rows, width), bf),
            pltpu.VMEM((heads, 2 * SEG, (LEFT + 2) * SEG), f32),
            pltpu.VMEM((rows, cols), bf),
            pltpu.VMEM((2 * rows, cols), bf),
            pltpu.VMEM((2 * rows, cols), bf),
            pltpu.VMEM((8, 2 * rows), jnp.int32),
            pltpu.VMEM((rows, cols), bf),
            pltpu.VMEM((2, rows, chunk), bf),
            pltpu.VMEM((2, rows, chunk), bf),
            pltpu.VMEM((rows, chunk), bf),
            pltpu.VMEM((rows, chunk), bf),
            pltpu.VMEM((n_tp, rows, chunk), bf),
            dma((4,)),
            dma((3, 4, n_sp)),
            dma((4, n_sp)),
            dma((3,)),
            dma((3,)),
            dma((6,)),
            dma((6,)),
            dma((n_tp,)),
        ],
        compiler_params=pltpu.CompilerParams(
            collective_id=0, has_side_effects=True, vmem_limit_bytes=48 * 1024 * 1024
        ),
    )(tokens, doc_col, doc_row, norm_gain, line, w_key[0], w_value[0], w_query[0], w_out[0])


def fits_one(mesh):
    return mesh.shape["sp"] % 2 == 0 and mesh.shape["sp"] <= 8 and mesh.shape["tp"] == 4


def solution(mesh):
    n_sp, n_tp = mesh.shape["sp"], mesh.shape["tp"]
    run = functools.partial(body_one, n_sp, n_tp) if fits_one(mesh) else body
    in_specs = (
        P("sp", None),
        P("sp"),
        P(),
        P(None, "sp", "tp"),
        P(None, "sp", "tp"),
        P(None, "sp", "tp"),
        P(None, None, "sp"),
        P(None, "tp", None),
    )
    out_specs = P("sp", None)
    return jax.shard_map(run, mesh=mesh, in_specs=in_specs, out_specs=out_specs, check_vma=False)
```

```python
import functools

import jax
import jax.numpy as jnp
from jax import lax
from jax.experimental import pallas as pl
from jax.experimental.pallas import tpu as pltpu
from jax.sharding import PartitionSpec as P

HEAD_DIM = 64
SEG = 64
LEFT = 4
REL_CLIP = 128


EPS = 1e-06


def passed_along(x, axis, by):
    length = lax.axis_size(axis)
    pairs = [(i, i + by) for i in range(length) if 0 <= i + by < length]
    return lax.ppermute(x, axis, pairs)


def banded_bias(bias_table, query_rows, key_rows, reach_rows):
    span_len = query_rows + key_rows - 1
    steps_back = jnp.arange(span_len, dtype=jnp.int32) - (key_rows - 1) + reach_rows
    lookup = jnp.clip(steps_back, -REL_CLIP, REL_CLIP) + REL_CLIP
    bias_line = jnp.take(bias_table, lookup, axis=1)
    reversed_line = bias_line[:, ::-1]
    repeated = jnp.tile(reversed_line, (1, query_rows))
    skewed = repeated[:, query_rows - 1 : query_rows - 1 + query_rows * (span_len - 1)]
    skewed = skewed.reshape(bias_table.shape[0], query_rows, span_len - 1)
    return skewed[:, :, :key_rows]


def attend(queries, keys_all, values_all, query_pos, key_pos, query_doc, key_doc, bias_table):
    query_rows = queries.shape[0]
    key_rows = keys_all.shape[0]
    reach_rows = key_rows - query_rows
    scores = jnp.einsum(
        "qhe,khe->hqk", queries, keys_all, preferred_element_type=jnp.float32
    ) * HEAD_DIM ** (-0.5)
    scores = scores + banded_bias(bias_table, query_rows, key_rows, reach_rows)
    query_seg = query_pos // SEG
    key_seg = key_pos // SEG
    allowed = (
        (key_pos[None, :] >= 0)
        & (key_seg[None, :] <= query_seg[:, None])
        & (key_seg[None, :] >= query_seg[:, None] - LEFT)
        & (key_doc[None, :] == query_doc[:, None])
    )
    scores = jnp.where(allowed[None], scores, -1e30)
    peak = jnp.max(scores, axis=-1, keepdims=True)
    raised = jnp.exp(scores - peak)
    weights_bf = (raised / jnp.sum(raised, axis=-1, keepdims=True)).astype(jnp.bfloat16)
    return jnp.einsum(
        "hqk,khe->qhe", weights_bf, values_all, preferred_element_type=jnp.float32
    ).astype(jnp.bfloat16)


def body(tokens, documents, norm_gain, w_query, w_key, w_value, w_out, rel_bias):
    local_rows = tokens.shape[0]
    reach_rows = LEFT * SEG
    width_local = w_query.shape[2]
    heads_local = width_local // HEAD_DIM
    offset = lax.axis_index("sp") * local_rows
    query_pos = offset + jnp.arange(local_rows, dtype=jnp.int32)
    key_pos = offset - reach_rows + jnp.arange(reach_rows + local_rows, dtype=jnp.int32)
    widened = tokens.astype(jnp.float32)
    normed = (
        widened
        * lax.rsqrt(jnp.mean(widened * widened, axis=-1, keepdims=True) + EPS)
        * norm_gain[0]
    ).astype(jnp.bfloat16)
    query_sum = jnp.dot(
        normed,
        lax.all_gather(w_query[0], "sp", axis=0, tiled=True),
        preferred_element_type=jnp.float32,
    )
    key_sum = jnp.dot(
        normed,
        lax.all_gather(w_key[0], "sp", axis=0, tiled=True),
        preferred_element_type=jnp.float32,
    )
    value_sum = jnp.dot(
        normed,
        lax.all_gather(w_value[0], "sp", axis=0, tiled=True),
        preferred_element_type=jnp.float32,
    )
    queries = query_sum.astype(jnp.bfloat16)
    keys_own = key_sum.astype(jnp.bfloat16)
    values_own = value_sum.astype(jnp.bfloat16)
    prior_keys, prior_values, prior_docs = passed_along((keys_own, values_own, documents), "sp", 1)
    keys_all = jnp.concatenate([prior_keys, keys_own], axis=0)
    values_all = jnp.concatenate([prior_values, values_own], axis=0)
    key_doc = jnp.concatenate([prior_docs, documents], axis=0)
    attended = attend(
        queries.reshape(local_rows, heads_local, HEAD_DIM),
        keys_all.reshape(reach_rows + local_rows, heads_local, HEAD_DIM),
        values_all.reshape(reach_rows + local_rows, heads_local, HEAD_DIM),
        query_pos,
        key_pos,
        documents,
        key_doc,
        rel_bias[0],
    ).reshape(local_rows, width_local)
    all_heads = lax.all_gather(attended, "tp", axis=1, tiled=True)
    return (
        widened
        + jnp.dot(
            all_heads,
            lax.all_gather(w_out[0], "sp", axis=1, tiled=True),
            preferred_element_type=jnp.float32,
        )
    ).astype(jnp.bfloat16)


MESH = pl.DeviceIdType.MESH
KEY, VALUE, QUERY, OUT = range(4)
UP, DOWN, ACROSS = range(3)
NEG = -1e30


def layer_kernel(
    n_sp, n_tp, doc_col, doc_row, gain_ref, line_ref, x_in, wk_in, wv_in, wq_in, wo_in, out_ref,
    w_all, w_mate, wo_all, x_ref, x_mate, normed, bias, q_buf, k_all, v_all, docs_all, docs_col, att, att_mate,
    part_out, part_in, hop_out, hop_in, done,
    own_sem, mate_sem, x_sem, send_sem, recv_sem, swap_send, swap_recv, halo_send, halo_recv,
    tp_send, tp_recv, store_sem,
):
    rows, width = x_ref.shape
    depth, cols = wk_in.shape
    half_cols = cols // 2
    chunk = width // n_tp
    lanes = 2 * HEAD_DIM
    nz = n_sp // 2
    s = lax.axis_index("sp")
    t = lax.axis_index("tp")
    z, x = s // 2, s % 2
    mate = s + 1 - 2 * x
    ty, tc = t // 2, t % 2
    t_core = t + 1 - 2 * tc
    t_y = (1 - ty) * 2 + tc
    own_in = (wk_in, wv_in, wq_in)

    def slot(kind, block):
        if kind == OUT:
            return wo_all.at[block]
        return w_all.at[kind, pl.ds(pl.multiple_of(block * depth, depth), depth), :]

    def column_half(kind, which):
        return own_in[kind].at[:, pl.ds(pl.multiple_of(which * half_cols, half_cols), half_cols)]

    def own_copy(kind):
        if kind == OUT:
            src = wo_in.at[pl.ds(pl.multiple_of(t * cols, cols), cols), :]
        else:
            src = column_half(kind, x)
        return pltpu.make_async_copy(src, slot(kind, s), own_sem.at[kind])

    def mate_copy(kind):
        return pltpu.make_async_copy(column_half(kind, 1 - x), w_mate.at[kind], mate_sem.at[kind])

    x_copy = pltpu.make_async_copy(x_in, x_ref, x_sem)
    for kind in range(3):
        own_copy(kind).start()
        mate_copy(kind).start()
    x_copy.start()
    own_copy(OUT).start()

    def move(way, kind, block):
        target = (s + 2, s - 2, mate)[way]
        src = slot(kind, block)
        if way == ACROSS and kind != OUT:
            src = w_mate.at[kind]
        return pltpu.make_async_remote_copy(
            src_ref=src, dst_ref=slot(kind, block),
            send_sem=send_sem.at[way, kind, block], recv_sem=recv_sem.at[kind, block],
            device_id={"sp": target}, device_id_type=MESH,
        )

    def halo(i):
        buf = (k_all, v_all, docs_all)[i]
        if i == 2:
            src, dst = buf.at[:, pl.ds(2 * rows, rows)], buf.at[:, pl.ds(0, rows)]
        else:
            src, dst = buf.at[pl.ds(2 * rows, rows), :], buf.at[pl.ds(0, rows), :]
        return pltpu.make_async_remote_copy(
            src_ref=src, dst_ref=dst, send_sem=halo_send.at[i], recv_sem=halo_recv.at[i],
            device_id={"sp": s + 2}, device_id_type=MESH,
        )

    def block_of(which):
        return pl.ds(pl.multiple_of(which * rows, rows), rows)

    def swap(i, src, dst):
        return pltpu.make_async_remote_copy(
            src_ref=src, dst_ref=dst, send_sem=swap_send.at[i], recv_sem=swap_recv.at[i],
            device_id={"sp": mate}, device_id_type=MESH,
        )

    x_swap = swap(0, x_ref, x_mate)
    row_swap = swap(1, doc_row, docs_all.at[:, block_of(1 + x)])
    col_swap = swap(2, doc_col, docs_col.at[block_of(x), :])
    att_half = pl.ds(pl.multiple_of(x * half_cols, half_cols), half_cols)
    att_swap = swap(3, att_mate, att.at[:, att_half])

    has_up, has_down = z < nz - 1, z > 0

    barrier = pltpu.get_barrier_semaphore()
    for peer in (mate, lax.rem(s + 2, n_sp), lax.rem(s + n_sp - 2, n_sp)):
        pl.semaphore_signal(barrier, inc=1, device_id={"sp": peer}, device_id_type=MESH)
    for peer in (t_core, t_y):
        pl.semaphore_signal(barrier, inc=1, device_id={"tp": peer}, device_id_type=MESH)
    pl.semaphore_wait(barrier, 5)

    def along_z(kind, block):
        pl.when(has_up)(lambda: move(UP, kind, block).start())
        pl.when(has_down)(lambda: move(DOWN, kind, block).start())

    def send_own(kind):
        own_copy(kind).wait()
        along_z(kind, s)
        if kind == OUT:
            move(ACROSS, kind, s).start()

    def send_mate(kind):
        mate_copy(kind).wait()
        move(ACROSS, kind, s).start()

    def forward_mate(kind):
        move(ACROSS, kind, mate).wait_recv()
        along_z(kind, mate)

    def columns(kind):
        return (s,) if kind == OUT else (s, mate)

    def forward(kind, d):
        for start in columns(kind):
            @pl.when(z - d >= 0)
            def _():
                block = start - 2 * d
                move(UP, kind, block).wait_recv()
                pl.when(has_up)(lambda: move(UP, kind, block).start())
                if kind == OUT:
                    move(ACROSS, kind, block).start()

            @pl.when(z + d < nz)
            def _():
                block = start + 2 * d
                move(DOWN, kind, block).wait_recv()
                pl.when(has_down)(lambda: move(DOWN, kind, block).start())
                if kind == OUT:
                    move(ACROSS, kind, block).start()

    def normalize(src, which):
        wide = src[...].astype(jnp.float32)
        normed[block_of(which), :] = (
            wide * lax.rsqrt(jnp.mean(wide * wide, axis=-1, keepdims=True) + EPS) * gain_ref[...]
        ).astype(jnp.bfloat16)

    send_mate(KEY)
    send_own(KEY)
    send_mate(VALUE)
    send_own(VALUE)
    send_mate(QUERY)
    x_copy.wait()
    x_swap.start()
    row_swap.start()
    col_swap.start()

    docs_all[:, block_of(1 + x)] = doc_row[...]
    docs_col[block_of(x), :] = doc_col[...]

    @pl.when(z == 0)
    def _():
        docs_all[:, pl.ds(0, rows)] = jnp.full((8, rows), -1, jnp.int32)
        k_all[pl.ds(0, rows), :] = jnp.zeros((rows, half_cols), jnp.bfloat16)
        v_all[pl.ds(0, rows), :] = jnp.zeros((rows, half_cols), jnp.bfloat16)

    forward_mate(KEY)
    normalize(x_ref, x)
    forward(KEY, 1)

    q_rows, span = 2 * SEG, (LEFT + 2) * SEG
    heads = half_cols // HEAD_DIM
    q_seg = lax.broadcasted_iota(jnp.int32, (q_rows, span), 0) // SEG
    k_seg = lax.broadcasted_iota(jnp.int32, (q_rows, span), 1) // SEG
    near = (k_seg >= q_seg) & (k_seg <= q_seg + LEFT)
    for h in range(heads):
        line = jnp.broadcast_to(line_ref[pl.ds(x * heads + h, 1), :], (q_rows, line_ref.shape[1]))
        skew = pltpu.roll(line, 0, 1, stride=1, stride_axis=0)
        bias[h] = jnp.where(near, skew[:, :span], NEG)

    def project(kind):
        return jnp.dot(normed[...], w_all[kind], preferred_element_type=jnp.float32)

    forward_mate(VALUE)
    for d in range(2, nz):
        forward(KEY, d)
    send_own(QUERY)
    forward_mate(QUERY)
    forward(VALUE, 1)
    x_swap.wait_recv()
    normalize(x_mate, 1 - x)
    for d in range(2, nz):
        forward(VALUE, d)
    k_all[pl.ds(rows, 2 * rows), :] = project(KEY).astype(jnp.bfloat16)
    row_swap.wait_recv()
    col_swap.wait_recv()
    forward(QUERY, 1)
    pl.when(has_up)(lambda: halo(0).start())
    pl.when(has_up)(lambda: halo(2).start())
    v_all[pl.ds(rows, 2 * rows), :] = project(VALUE).astype(jnp.bfloat16)
    for d in range(2, nz - 1):
        forward(QUERY, d)
    pl.when(has_up)(lambda: halo(1).start())
    send_own(OUT)
    forward(QUERY, nz - 1)
    q_buf[...] = (project(QUERY).astype(jnp.bfloat16).astype(jnp.float32) * HEAD_DIM ** (-0.5)).astype(jnp.bfloat16)

    @pl.when(has_down)
    def _():
        for i in range(3):
            halo(i).wait_recv()

    low = lax.broadcasted_iota(jnp.int32, (q_rows, lanes), 1) < HEAD_DIM

    def attend_rows(which, j):
        first = pl.multiple_of(which * rows + j * q_rows, q_rows)
        queries, keys = pl.ds(first, q_rows), pl.ds(first, span)
        same = docs_col[queries, :][:, :1] == docs_all[pl.ds(0, 1), keys]
        found = []
        for p in range(half_cols // lanes):
            q_pair = q_buf[queries, pl.ds(p * lanes, lanes)]
            k_pair = k_all[keys, pl.ds(p * lanes, lanes)]
            v_pair = v_all[keys, pl.ds(p * lanes, lanes)]
            both = []
            for half in range(2):
                mine = low if half == 0 else jnp.logical_not(low)
                q_one = jnp.where(mine, q_pair, jnp.zeros_like(q_pair))
                score = lax.dot_general(
                    q_one, k_pair, (((1,), (1,)), ((), ())), preferred_element_type=jnp.float32
                )
                score = jnp.where(same, score + bias[2 * p + half], NEG)
                raised = jnp.exp(score - jnp.max(score, axis=-1, keepdims=True))
                total = jnp.sum(raised, axis=-1, keepdims=True)
                both.append(
                    jnp.dot(raised.astype(jnp.bfloat16), v_pair, preferred_element_type=jnp.float32) / total
                )
            found.append(jnp.where(low, both[0], both[1]).astype(jnp.bfloat16))
        return jnp.concatenate(found, axis=1)

    parts = rows // q_rows
    for j in range(parts):
        att_mate[pl.ds(j * q_rows, q_rows), :] = attend_rows(1 - x, j)
    forward(OUT, 1)
    for j in range(parts):
        att[pl.ds(j * q_rows, q_rows), att_half] = attend_rows(x, j)
        if j == 0:
            att_swap.start()
            forward(OUT, 2)
    for d in range(3, nz):
        forward(OUT, d)
    for d in range(nz):
        move(ACROSS, OUT, 2 * d + 1 - x).wait_recv()
    att_swap.wait_recv()

    def product(block):
        return jnp.dot(att[...], wo_all[block], preferred_element_type=jnp.float32)

    def chunk_product(which):
        each = chunk // wo_in.shape[1]
        return jnp.concatenate([product(which * each + i) for i in range(each)], axis=1)

    def tp_move(i, src, dst, target):
        return pltpu.make_async_remote_copy(
            src_ref=src, dst_ref=dst, send_sem=tp_send.at[i], recv_sem=tp_recv.at[i],
            device_id={"tp": target}, device_id_type=MESH,
        )

    part_moves = [tp_move(i, part_out.at[i], part_in.at[i], t_core) for i in range(2)]
    for i in range(2):
        other = (1 - ty if i == 0 else ty) * 2 + (1 - tc)
        part_out[i] = chunk_product(other).astype(jnp.bfloat16)
        part_moves[i].start()
    far = chunk_product(t_y)
    part_moves[0].wait_recv()
    hop_out[...] = (far + part_in[0].astype(jnp.float32)).astype(jnp.bfloat16)
    hop = tp_move(2, hop_out, hop_in, t_y)
    hop.start()
    near_sum = chunk_product(t)
    part_moves[1].wait_recv()
    near_sum = near_sum + part_in[1].astype(jnp.float32)
    near_sum = near_sum + x_ref[:, pl.ds(pl.multiple_of(t * chunk, chunk), chunk)].astype(jnp.float32)
    hop.wait_recv()
    done[t] = (near_sum + hop_in[...].astype(jnp.float32)).astype(jnp.bfloat16)

    def store(which):
        return pltpu.make_async_copy(
            done.at[which], out_ref.at[:, pl.ds(pl.multiple_of(which * chunk, chunk), chunk)], store_sem.at[which]
        )

    far_core = (1 - ty) * 2 + (1 - tc)
    to_y = tp_move(3, done.at[t], done.at[t], t_y)
    to_core = tp_move(4, done.at[t], done.at[t], t_core)
    pass_on = tp_move(5, done.at[t_y], done.at[t_y], t_core)
    to_y.start()
    to_core.start()
    store(t).start()
    to_y.wait_recv()
    pass_on.start()
    store(t_y).start()
    to_core.wait_recv()
    store(t_core).start()
    pass_on.wait_recv()
    store(far_core).start()
    for which in range(n_tp):
        store(which).wait()

    for kind in range(4):
        if kind != OUT:
            move(ACROSS, kind, s).wait_send()
        for start in columns(kind):
            for d in range(nz):
                @pl.when(z - d >= 0)
                def _():
                    pl.when(has_up)(lambda: move(UP, kind, start - 2 * d).wait_send())
                    if kind == OUT:
                        move(ACROSS, kind, start - 2 * d).wait_send()

                @pl.when(z + d < nz)
                def _():
                    pl.when(has_down)(lambda: move(DOWN, kind, start + 2 * d).wait_send())
                    if kind == OUT and d:
                        move(ACROSS, kind, start + 2 * d).wait_send()

    @pl.when(has_up)
    def _():
        for i in range(3):
            halo(i).wait_send()
    for one in (x_swap, row_swap, col_swap, att_swap, *part_moves, hop, to_y, to_core, pass_on):
        one.wait_send()


def body_one(n_sp, n_tp, tokens, documents, norm_gain, w_query, w_key, w_value, w_out, rel_bias):
    rows, width = tokens.shape
    depth, cols = w_query.shape[1:]
    heads = cols // HEAD_DIM
    out_cols = w_out.shape[2]
    chunk = width // n_tp
    reach = LEFT * SEG
    table = rel_bias[0]
    furthest = table[:, 2 * REL_CLIP:]
    ahead, behind = reach - REL_CLIP, reach - REL_CLIP - 1
    line = jnp.concatenate(
        [
            jnp.broadcast_to(furthest, (heads, ahead)),
            table[:, ::-1],
            jnp.broadcast_to(furthest, (heads, behind)),
        ],
        axis=1,
    )
    doc_col = jnp.broadcast_to(documents[:, None], (rows, 128))
    doc_row = jnp.broadcast_to(documents[None, :], (8, rows))
    bf, f32 = jnp.bfloat16, jnp.float32
    vmem = pl.BlockSpec(memory_space=pltpu.VMEM)
    hbm = pl.BlockSpec(memory_space=pl.ANY)
    dma = pltpu.SemaphoreType.DMA
    return pl.pallas_call(
        functools.partial(layer_kernel, n_sp, n_tp),
        out_shape=jax.ShapeDtypeStruct((rows, width), bf),
        in_specs=[vmem] * 4 + [hbm] * 5,
        out_specs=hbm,
        scratch_shapes=[
            pltpu.VMEM((3, n_sp * depth, cols // 2), bf),
            pltpu.VMEM((3, depth, cols // 2), bf),
            pltpu.VMEM((n_sp, cols, out_cols), bf),
            pltpu.VMEM((rows, width), bf),
            pltpu.VMEM((rows, width), bf),
            pltpu.VMEM((2 * rows, width), bf),
            pltpu.VMEM((heads // 2, 2 * SEG, (LEFT + 2) * SEG), f32),
            pltpu.VMEM((2 * rows, cols // 2), bf),
            pltpu.VMEM((3 * rows, cols // 2), bf),
            pltpu.VMEM((3 * rows, cols // 2), bf),
            pltpu.VMEM((8, 3 * rows), jnp.int32),
            pltpu.VMEM((2 * rows, 128), jnp.int32),
            pltpu.VMEM((rows, cols), bf),
            pltpu.VMEM((rows, cols // 2), bf),
            pltpu.VMEM((2, rows, chunk), bf),
            pltpu.VMEM((2, rows, chunk), bf),
            pltpu.VMEM((rows, chunk), bf),
            pltpu.VMEM((rows, chunk), bf),
            pltpu.VMEM((n_tp, rows, chunk), bf),
            dma((4,)),
            dma((3,)),
            dma(()),
            dma((3, 4, n_sp)),
            dma((4, n_sp)),
            dma((4,)),
            dma((4,)),
            dma((3,)),
            dma((3,)),
            dma((6,)),
            dma((6,)),
            dma((n_tp,)),
        ],
        compiler_params=pltpu.CompilerParams(
            collective_id=0, has_side_effects=True, vmem_limit_bytes=60 * 1024 * 1024
        ),
    )(doc_col, doc_row, norm_gain, line, tokens, w_key[0], w_value[0], w_query[0], w_out[0])


def fits_one(mesh):
    return mesh.shape["sp"] % 2 == 0 and 6 <= mesh.shape["sp"] <= 8 and mesh.shape["tp"] == 4


def solution(mesh):
    n_sp, n_tp = mesh.shape["sp"], mesh.shape["tp"]
    run = functools.partial(body_one, n_sp, n_tp) if fits_one(mesh) else body
    in_specs = (
        P("sp", None),
        P("sp"),
        P(),
        P(None, "sp", "tp"),
        P(None, "sp", "tp"),
        P(None, "sp", "tp"),
        P(None, None, "sp"),
        P(None, "tp", None),
    )
    out_specs = P("sp", None)
    return jax.shard_map(run, mesh=mesh, in_specs=in_specs, out_specs=out_specs, check_vma=False)
```

```python
import functools

import jax
import jax.numpy as jnp
from jax import lax
from jax.experimental import pallas as pl
from jax.experimental.pallas import tpu as pltpu
from jax.sharding import PartitionSpec as P

HEAD_DIM = 64
SEG = 64
LEFT = 4
REL_CLIP = 128


EPS = 1e-06


def passed_along(x, axis, by):
    length = lax.axis_size(axis)
    pairs = [(i, i + by) for i in range(length) if 0 <= i + by < length]
    return lax.ppermute(x, axis, pairs)


def banded_bias(bias_table, query_rows, key_rows, reach_rows):
    span_len = query_rows + key_rows - 1
    steps_back = jnp.arange(span_len, dtype=jnp.int32) - (key_rows - 1) + reach_rows
    lookup = jnp.clip(steps_back, -REL_CLIP, REL_CLIP) + REL_CLIP
    bias_line = jnp.take(bias_table, lookup, axis=1)
    reversed_line = bias_line[:, ::-1]
    repeated = jnp.tile(reversed_line, (1, query_rows))
    skewed = repeated[:, query_rows - 1 : query_rows - 1 + query_rows * (span_len - 1)]
    skewed = skewed.reshape(bias_table.shape[0], query_rows, span_len - 1)
    return skewed[:, :, :key_rows]


def attend(queries, keys_all, values_all, query_pos, key_pos, query_doc, key_doc, bias_table):
    query_rows = queries.shape[0]
    key_rows = keys_all.shape[0]
    reach_rows = key_rows - query_rows
    scores = jnp.einsum(
        "qhe,khe->hqk", queries, keys_all, preferred_element_type=jnp.float32
    ) * HEAD_DIM ** (-0.5)
    scores = scores + banded_bias(bias_table, query_rows, key_rows, reach_rows)
    query_seg = query_pos // SEG
    key_seg = key_pos // SEG
    allowed = (
        (key_pos[None, :] >= 0)
        & (key_seg[None, :] <= query_seg[:, None])
        & (key_seg[None, :] >= query_seg[:, None] - LEFT)
        & (key_doc[None, :] == query_doc[:, None])
    )
    scores = jnp.where(allowed[None], scores, -1e30)
    peak = jnp.max(scores, axis=-1, keepdims=True)
    raised = jnp.exp(scores - peak)
    weights_bf = (raised / jnp.sum(raised, axis=-1, keepdims=True)).astype(jnp.bfloat16)
    return jnp.einsum(
        "hqk,khe->qhe", weights_bf, values_all, preferred_element_type=jnp.float32
    ).astype(jnp.bfloat16)


def body(tokens, documents, norm_gain, w_query, w_key, w_value, w_out, rel_bias):
    local_rows = tokens.shape[0]
    reach_rows = LEFT * SEG
    width_local = w_query.shape[2]
    heads_local = width_local // HEAD_DIM
    offset = lax.axis_index("sp") * local_rows
    query_pos = offset + jnp.arange(local_rows, dtype=jnp.int32)
    key_pos = offset - reach_rows + jnp.arange(reach_rows + local_rows, dtype=jnp.int32)
    widened = tokens.astype(jnp.float32)
    normed = (
        widened
        * lax.rsqrt(jnp.mean(widened * widened, axis=-1, keepdims=True) + EPS)
        * norm_gain[0]
    ).astype(jnp.bfloat16)
    query_sum = jnp.dot(
        normed,
        lax.all_gather(w_query[0], "sp", axis=0, tiled=True),
        preferred_element_type=jnp.float32,
    )
    key_sum = jnp.dot(
        normed,
        lax.all_gather(w_key[0], "sp", axis=0, tiled=True),
        preferred_element_type=jnp.float32,
    )
    value_sum = jnp.dot(
        normed,
        lax.all_gather(w_value[0], "sp", axis=0, tiled=True),
        preferred_element_type=jnp.float32,
    )
    queries = query_sum.astype(jnp.bfloat16)
    keys_own = key_sum.astype(jnp.bfloat16)
    values_own = value_sum.astype(jnp.bfloat16)
    prior_keys, prior_values, prior_docs = passed_along((keys_own, values_own, documents), "sp", 1)
    keys_all = jnp.concatenate([prior_keys, keys_own], axis=0)
    values_all = jnp.concatenate([prior_values, values_own], axis=0)
    key_doc = jnp.concatenate([prior_docs, documents], axis=0)
    attended = attend(
        queries.reshape(local_rows, heads_local, HEAD_DIM),
        keys_all.reshape(reach_rows + local_rows, heads_local, HEAD_DIM),
        values_all.reshape(reach_rows + local_rows, heads_local, HEAD_DIM),
        query_pos,
        key_pos,
        documents,
        key_doc,
        rel_bias[0],
    ).reshape(local_rows, width_local)
    all_heads = lax.all_gather(attended, "tp", axis=1, tiled=True)
    return (
        widened
        + jnp.dot(
            all_heads,
            lax.all_gather(w_out[0], "sp", axis=1, tiled=True),
            preferred_element_type=jnp.float32,
        )
    ).astype(jnp.bfloat16)


MESH = pl.DeviceIdType.MESH
KEY, VALUE, QUERY, OUT = range(4)
UP, DOWN, ACROSS = range(3)
NEG = -1e30


def layer_kernel(
    n_sp, n_tp, doc_col, doc_row, gain_ref, line_ref, x_in, wk_in, wv_in, wq_in, wo_in, out_ref,
    w_all, w_mate, wo_all, x_ref, x_mate, normed, bias, q_buf, k_all, v_all, docs_all, docs_col, att, att_mate, done,
    own_sem, out_sem, mate_sem, x_sem, send_sem, recv_sem, swap_send, swap_recv, halo_send, halo_recv,
    tp_send, tp_recv, store_sem,
):
    rows, width = x_ref.shape
    depth, cols = wk_in.shape
    half_cols = cols // 2
    chunk = width // n_tp
    lanes = 2 * HEAD_DIM
    nz = n_sp // 2
    s = lax.axis_index("sp")
    t = lax.axis_index("tp")
    z, x = s // 2, s % 2
    mate = s + 1 - 2 * x
    ty, tc = t // 2, t % 2
    t_core = t + 1 - 2 * tc
    t_y = (1 - ty) * 2 + tc
    own_in = (wk_in, wv_in, wq_in)

    def slot(kind, block):
        if kind == OUT:
            return wo_all.at[block]
        return w_all.at[kind, pl.ds(pl.multiple_of(block * depth, depth), depth), :]

    def column_half(kind, which):
        return own_in[kind].at[:, pl.ds(pl.multiple_of(which * half_cols, half_cols), half_cols)]

    def own_copy(kind):
        return pltpu.make_async_copy(column_half(kind, x), slot(kind, s), own_sem.at[kind])

    def out_copy(r):
        return pltpu.make_async_copy(wo_in.at[pl.ds(r * cols, cols), :], slot(OUT, 2 * r + x), out_sem.at[r])

    def mate_copy(kind):
        return pltpu.make_async_copy(column_half(kind, 1 - x), w_mate.at[kind], mate_sem.at[kind])

    x_copy = pltpu.make_async_copy(x_in, x_ref, x_sem)
    for kind in range(3):
        own_copy(kind).start()
        mate_copy(kind).start()
    x_copy.start()

    @pl.when(z == t)
    def _():
        for r in range(n_tp):
            out_copy(r).start()


    def move(way, kind, block):
        target = (s + 2, s - 2, mate)[way]
        src = slot(kind, block)
        if way == ACROSS and kind != OUT:
            src = w_mate.at[kind]
        return pltpu.make_async_remote_copy(
            src_ref=src, dst_ref=slot(kind, block),
            send_sem=send_sem.at[way, kind, block], recv_sem=recv_sem.at[kind, block],
            device_id={"sp": target}, device_id_type=MESH,
        )

    def halo(i):
        buf = (k_all, v_all, docs_all)[i]
        if i == 2:
            src, dst = buf.at[:, pl.ds(2 * rows, rows)], buf.at[:, pl.ds(0, rows)]
        else:
            src, dst = buf.at[pl.ds(2 * rows, rows), :], buf.at[pl.ds(0, rows), :]
        return pltpu.make_async_remote_copy(
            src_ref=src, dst_ref=dst, send_sem=halo_send.at[i], recv_sem=halo_recv.at[i],
            device_id={"sp": s + 2}, device_id_type=MESH,
        )

    def block_of(which):
        return pl.ds(pl.multiple_of(which * rows, rows), rows)

    def swap(i, src, dst):
        return pltpu.make_async_remote_copy(
            src_ref=src, dst_ref=dst, send_sem=swap_send.at[i], recv_sem=swap_recv.at[i],
            device_id={"sp": mate}, device_id_type=MESH,
        )

    x_swap = swap(0, x_ref, x_mate)
    row_swap = swap(1, doc_row, docs_all.at[:, block_of(1 + x)])
    col_swap = swap(2, doc_col, docs_col.at[block_of(x), :])
    att_half = pl.ds(pl.multiple_of(x * half_cols, half_cols), half_cols)
    att_swap = swap(3, att_mate, att.at[t, :, att_half])

    has_up, has_down = z < nz - 1, z > 0

    barrier = pltpu.get_barrier_semaphore()
    for peer in (mate, lax.rem(s + 2, n_sp), lax.rem(s + n_sp - 2, n_sp)):
        pl.semaphore_signal(barrier, inc=1, device_id={"sp": peer}, device_id_type=MESH)
    for peer in (t_core, t_y):
        pl.semaphore_signal(barrier, inc=1, device_id={"tp": peer}, device_id_type=MESH)
    pl.semaphore_wait(barrier, 5)

    def along_z(kind, block):
        pl.when(has_up)(lambda: move(UP, kind, block).start())
        pl.when(has_down)(lambda: move(DOWN, kind, block).start())

    def send_own(kind):
        own_copy(kind).wait()
        along_z(kind, s)

    def send_mate(kind):
        mate_copy(kind).wait()
        move(ACROSS, kind, s).start()

    def forward_mate(kind):
        move(ACROSS, kind, mate).wait_recv()
        along_z(kind, mate)

    def forward(kind, d):
        for start in (s, mate):
            @pl.when(z - d >= 0)
            def _():
                block = start - 2 * d
                move(UP, kind, block).wait_recv()
                pl.when(has_up)(lambda: move(UP, kind, block).start())

            @pl.when(z + d < nz)
            def _():
                block = start + 2 * d
                move(DOWN, kind, block).wait_recv()
                pl.when(has_down)(lambda: move(DOWN, kind, block).start())

    sends_up, sends_down = (z >= t) & has_up, (z <= t) & has_down

    def send_out(r):
        pl.when(sends_up)(lambda: move(UP, OUT, 2 * r + x).start())
        pl.when(sends_down)(lambda: move(DOWN, OUT, 2 * r + x).start())
        move(ACROSS, OUT, 2 * r + x).start()

    def forward_out(r):
        @pl.when(z != t)
        def _():
            move(UP, OUT, 2 * r + x).wait_recv()
            send_out(r)

    def normalize(src, which):
        wide = src[...].astype(jnp.float32)
        normed[block_of(which), :] = (
            wide * lax.rsqrt(jnp.mean(wide * wide, axis=-1, keepdims=True) + EPS) * gain_ref[...]
        ).astype(jnp.bfloat16)

    send_mate(KEY)
    send_own(KEY)
    send_mate(VALUE)
    send_own(VALUE)
    send_mate(QUERY)
    x_copy.wait()
    x_swap.start()
    row_swap.start()
    col_swap.start()

    docs_all[:, block_of(1 + x)] = doc_row[...]
    docs_col[block_of(x), :] = doc_col[...]

    @pl.when(z == 0)
    def _():
        docs_all[:, pl.ds(0, rows)] = jnp.full((8, rows), -1, jnp.int32)
        k_all[pl.ds(0, rows), :] = jnp.zeros((rows, half_cols), jnp.bfloat16)
        v_all[pl.ds(0, rows), :] = jnp.zeros((rows, half_cols), jnp.bfloat16)

    forward_mate(KEY)
    normalize(x_ref, x)
    forward(KEY, 1)

    q_rows, span = 2 * SEG, (LEFT + 2) * SEG
    heads = half_cols // HEAD_DIM
    q_seg = lax.broadcasted_iota(jnp.int32, (q_rows, span), 0) // SEG
    k_seg = lax.broadcasted_iota(jnp.int32, (q_rows, span), 1) // SEG
    near = (k_seg >= q_seg) & (k_seg <= q_seg + LEFT)
    for h in range(heads):
        line = jnp.broadcast_to(line_ref[pl.ds(x * heads + h, 1), :], (q_rows, line_ref.shape[1]))
        skew = pltpu.roll(line, 0, 1, stride=1, stride_axis=0)
        bias[h] = jnp.where(near, skew[:, :span], NEG)

    def project(kind):
        return jnp.dot(normed[...], w_all[kind], preferred_element_type=jnp.float32)

    forward_mate(VALUE)
    for d in range(2, nz):
        forward(KEY, d)
    send_own(QUERY)
    forward_mate(QUERY)
    for d in range(1, nz):
        forward(VALUE, d)
    x_swap.wait_recv()
    normalize(x_mate, 1 - x)
    k_all[pl.ds(rows, 2 * rows), :] = project(KEY).astype(jnp.bfloat16)
    row_swap.wait_recv()
    col_swap.wait_recv()
    forward(QUERY, 1)
    pl.when(has_up)(lambda: halo(0).start())
    pl.when(has_up)(lambda: halo(2).start())
    v_all[pl.ds(rows, 2 * rows), :] = project(VALUE).astype(jnp.bfloat16)
    for d in range(2, nz - 1):
        forward(QUERY, d)
    pl.when(has_up)(lambda: halo(1).start())

    @pl.when(z == t)
    def _():
        for r in range(n_tp):
            out_copy(r).wait()
            send_out(r)

    forward(QUERY, nz - 1)
    q_buf[...] = (project(QUERY).astype(jnp.bfloat16).astype(jnp.float32) * HEAD_DIM ** (-0.5)).astype(jnp.bfloat16)

    @pl.when(has_down)
    def _():
        for i in range(3):
            halo(i).wait_recv()

    low = lax.broadcasted_iota(jnp.int32, (q_rows, lanes), 1) < HEAD_DIM

    def attend_rows(which, j):
        first = pl.multiple_of(which * rows + j * q_rows, q_rows)
        queries, keys = pl.ds(first, q_rows), pl.ds(first, span)
        same = docs_col[queries, :][:, :1] == docs_all[pl.ds(0, 1), keys]
        found = []
        for p in range(half_cols // lanes):
            q_pair = q_buf[queries, pl.ds(p * lanes, lanes)]
            k_pair = k_all[keys, pl.ds(p * lanes, lanes)]
            v_pair = v_all[keys, pl.ds(p * lanes, lanes)]
            both = []
            for half in range(2):
                mine = low if half == 0 else jnp.logical_not(low)
                q_one = jnp.where(mine, q_pair, jnp.zeros_like(q_pair))
                score = lax.dot_general(
                    q_one, k_pair, (((1,), (1,)), ((), ())), preferred_element_type=jnp.float32
                )
                score = jnp.where(same, score + bias[2 * p + half], NEG)
                raised = jnp.exp(score - jnp.max(score, axis=-1, keepdims=True))
                total = jnp.sum(raised, axis=-1, keepdims=True)
                both.append(
                    jnp.dot(raised.astype(jnp.bfloat16), v_pair, preferred_element_type=jnp.float32) / total
                )
            found.append(jnp.where(low, both[0], both[1]).astype(jnp.bfloat16))
        return jnp.concatenate(found, axis=1)

    def tp_move(i, ref, which, target):
        return pltpu.make_async_remote_copy(
            src_ref=ref.at[which], dst_ref=ref.at[which], send_sem=tp_send.at[i], recv_sem=tp_recv.at[i],
            device_id={"tp": target}, device_id_type=MESH,
        )

    att_y = tp_move(0, att, t, t_y)
    att_core = tp_move(1, att, t, t_core)
    att_on = tp_move(2, att, t_y, t_core)

    parts = rows // q_rows
    for j in range(parts):
        att_mate[pl.ds(j * q_rows, q_rows), :] = attend_rows(1 - x, j)
    forward_out(0)
    for j in range(parts):
        att[t, pl.ds(j * q_rows, q_rows), att_half] = attend_rows(x, j)
        if j == 0:
            att_swap.start()
    forward_out(1)
    att_swap.wait_recv()
    att_y.start()
    att_core.start()
    for r in range(2, n_tp):
        forward_out(r)
    att_y.wait_recv()
    att_on.start()
    att_core.wait_recv()
    att_on.wait_recv()
    for r in range(n_tp):
        move(ACROSS, OUT, 2 * r + 1 - x).wait_recv()
    sums = [x_ref[:, pl.ds(pl.multiple_of(t * chunk + i * (chunk // 2), chunk // 2), chunk // 2)].astype(jnp.float32) for i in range(2)]
    for i in range(2):
        made = jnp.zeros_like(sums[i])
        for r in range(n_tp):
            made = made + jnp.dot(att[r], wo_all[2 * r + i], preferred_element_type=jnp.float32)
        done[t, :, pl.ds(i * (chunk // 2), chunk // 2)] = (sums[i] + made).astype(jnp.bfloat16)

    def store(which):
        return pltpu.make_async_copy(
            done.at[which], out_ref.at[:, pl.ds(pl.multiple_of(which * chunk, chunk), chunk)], store_sem.at[which]
        )

    far_core = (1 - ty) * 2 + (1 - tc)
    to_y = tp_move(3, done, t, t_y)
    to_core = tp_move(4, done, t, t_core)
    pass_on = tp_move(5, done, t_y, t_core)
    to_y.start()
    to_core.start()
    store(t).start()
    to_y.wait_recv()
    pass_on.start()
    store(t_y).start()
    to_core.wait_recv()
    store(t_core).start()
    pass_on.wait_recv()
    store(far_core).start()
    for which in range(n_tp):
        store(which).wait()

    for kind in range(3):
        move(ACROSS, kind, s).wait_send()
        for start in (s, mate):
            for d in range(nz):
                @pl.when(z - d >= 0)
                def _():
                    pl.when(has_up)(lambda: move(UP, kind, start - 2 * d).wait_send())

                @pl.when(z + d < nz)
                def _():
                    pl.when(has_down)(lambda: move(DOWN, kind, start + 2 * d).wait_send())
    for r in range(n_tp):
        pl.when(sends_up)(lambda: move(UP, OUT, 2 * r + x).wait_send())
        pl.when(sends_down)(lambda: move(DOWN, OUT, 2 * r + x).wait_send())
        move(ACROSS, OUT, 2 * r + x).wait_send()

    @pl.when(has_up)
    def _():
        for i in range(3):
            halo(i).wait_send()
    for one in (x_swap, row_swap, col_swap, att_swap, att_y, att_core, att_on, to_y, to_core, pass_on):
        one.wait_send()


def body_one(n_sp, n_tp, tokens, documents, norm_gain, w_query, w_key, w_value, w_out, rel_bias):
    rows, width = tokens.shape
    depth, cols = w_query.shape[1:]
    heads = cols // HEAD_DIM
    out_cols = w_out.shape[2]
    chunk = width // n_tp
    reach = LEFT * SEG
    table = rel_bias[0]
    furthest = table[:, 2 * REL_CLIP:]
    ahead, behind = reach - REL_CLIP, reach - REL_CLIP - 1
    line = jnp.concatenate(
        [
            jnp.broadcast_to(furthest, (heads, ahead)),
            table[:, ::-1],
            jnp.broadcast_to(furthest, (heads, behind)),
        ],
        axis=1,
    )
    doc_col = jnp.broadcast_to(documents[:, None], (rows, 128))
    doc_row = jnp.broadcast_to(documents[None, :], (8, rows))
    bf, f32 = jnp.bfloat16, jnp.float32
    vmem = pl.BlockSpec(memory_space=pltpu.VMEM)
    hbm = pl.BlockSpec(memory_space=pl.ANY)
    dma = pltpu.SemaphoreType.DMA
    return pl.pallas_call(
        functools.partial(layer_kernel, n_sp, n_tp),
        out_shape=jax.ShapeDtypeStruct((rows, width), bf),
        in_specs=[vmem] * 4 + [hbm] * 5,
        out_specs=hbm,
        scratch_shapes=[
            pltpu.VMEM((3, n_sp * depth, cols // 2), bf),
            pltpu.VMEM((3, depth, cols // 2), bf),
            pltpu.VMEM((n_sp, cols, out_cols), bf),
            pltpu.VMEM((rows, width), bf),
            pltpu.VMEM((rows, width), bf),
            pltpu.VMEM((2 * rows, width), bf),
            pltpu.VMEM((heads // 2, 2 * SEG, (LEFT + 2) * SEG), f32),
            pltpu.VMEM((2 * rows, cols // 2), bf),
            pltpu.VMEM((3 * rows, cols // 2), bf),
            pltpu.VMEM((3 * rows, cols // 2), bf),
            pltpu.VMEM((8, 3 * rows), jnp.int32),
            pltpu.VMEM((2 * rows, 128), jnp.int32),
            pltpu.VMEM((n_tp, rows, cols), bf),
            pltpu.VMEM((rows, cols // 2), bf),
            pltpu.VMEM((n_tp, rows, chunk), bf),
            dma((3,)),
            dma((n_tp,)),
            dma((3,)),
            dma(()),
            dma((3, 4, n_sp)),
            dma((4, n_sp)),
            dma((4,)),
            dma((4,)),
            dma((3,)),
            dma((3,)),
            dma((6,)),
            dma((6,)),
            dma((n_tp,)),
        ],
        compiler_params=pltpu.CompilerParams(
            collective_id=0, has_side_effects=True, vmem_limit_bytes=60 * 1024 * 1024
        ),
    )(doc_col, doc_row, norm_gain, line, tokens, w_key[0], w_value[0], w_query[0], w_out[0])


def fits_one(mesh):
    return mesh.shape["tp"] == 4 and mesh.shape["sp"] == 2 * mesh.shape["tp"]


def solution(mesh):
    n_sp, n_tp = mesh.shape["sp"], mesh.shape["tp"]
    run = functools.partial(body_one, n_sp, n_tp) if fits_one(mesh) else body
    in_specs = (
        P("sp", None),
        P("sp"),
        P(),
        P(None, "sp", "tp"),
        P(None, "sp", "tp"),
        P(None, "sp", "tp"),
        P(None, None, "sp"),
        P(None, "tp", None),
    )
    out_specs = P("sp", None)
    return jax.shard_map(run, mesh=mesh, in_specs=in_specs, out_specs=out_specs, check_vma=False)
```
